32 devices in a mesh: ep: 16 (over z, x, core), tp: 2 (over y).
Axes of the slice: x: 2, y: 2, z: 4, core: 2. Of those that a mesh axis runs over, the one named last changes fastest.
Arguments:
- residual_in: bfloat16 [240, 1536], P('ep'), may hold values from -6 to 6
- rec_state: bfloat16 [240, 12, 128, 128], P('ep', 'tp'), may hold values from -6 to 6
- mix_gain: float32 [1536], replicated, may hold values from 0.1 to 1.9
- w_query: bfloat16 [1536, 1536], P('tp', 'ep'), may hold values from -0.15625 to 0.15625
- w_forget: bfloat16 [1536, 1536], P('tp', 'ep'), may hold values from -0.15625 to 0.15625
- w_input: bfloat16 [1536, 1536], P('tp', 'ep'), may hold values from -0.15625 to 0.15625
- w_gate: bfloat16 [1536, 1536], P('tp', 'ep'), may hold values from -0.15625 to 0.15625
- lower_bound: float32 [1536], P('tp'), may hold values from 0 to 0.9
- head_gain: float32 [128], replicated, may hold values from 0.1 to 1.9
- w_out: bfloat16 [1536, 1536], P('tp', 'ep'), may hold values from -0.15625 to 0.15625
- ffn_gain: float32 [1536], replicated, may hold values from 0.1 to 1.9
- route_ids: int32 [240, 6], P('ep'), may hold values from 0 to 15, all different within a row; in each aligned block of 15 rows (0 to 14, 15 to 29, ...) at most 6 rows name the same one
- route_weight: float32 [240, 6], P('ep'), may hold values from 0.2 to 1
- expert_gate: bfloat16 [16, 1536, 512], P('ep', None, 'tp'), may hold values from -0.15625 to 0.15625
- expert_up: bfloat16 [16, 1536, 512], P('ep', None, 'tp'), may hold values from -0.15625 to 0.15625
- expert_down: bfloat16 [16, 512, 1536], P('ep', 'tp'), may hold values from -0.25 to 0.25
Outputs:
- layer_out: bfloat16 [240, 1536], P('ep', 'tp')
- new_state: bfloat16 [240, 12, 128, 128], P('ep', 'tp')
The draws below stay inside these ranges and needn't reach their ends.
Inputs may be any that keep to these rules, and one draw needn't show every extreme that they name: `route_ids`: each row names 6 different experts. Among the rows of one device no expert is named more than 6 times, and in every draw some device names some expert exactly 6 times.
All inputs are finite; a program needn't handle non-finite values.
Results may differ from the reference program's by a relative error of at most 0.016.
Values may be sent and summed in bfloat16 or wider, within the bound.
A program may use at most 64 MiB of HBM per device.

```python
import math
import jax
import jax.numpy as jnp
import numpy as np
from jax import lax

D = 1536
HEADS = 12
FF = 512
TOPK = 6
SEQ_DEV = 15
HEAD = 128
TOKENS = 240
EXPERTS = 16
CAP = 6
N_EP = 16


def level_of(rng, dims, split, least, largest):
    level, own = 1.0, jax.random.fold_in(rng, 6)
    for position, shards_of in split:
        draws = jnp.exp(jax.random.uniform(jax.random.fold_in(own, position), (shards_of,), jnp.float32, least / len(split), largest / len(split)))
        level = level * jnp.repeat(draws, dims[position] // shards_of).reshape([-1 if axis == position else 1 for axis in range(len(dims))])
    return level


def shared_out(rng, own, number, rows, amount, top, bound, slope):
    ranking = jax.random.permutation(rng, amount)
    crowded, usual = shares(amount, rows * top, bound, slope, True), shares(amount, rows * top, bound, slope, False)
    places = jnp.arange(amount)

    def named(tallies, offset_by):
        used = int((tallies > 0).sum())
        fixed = max(1, used // 4)
        shifted = fixed + (places - fixed + offset_by * (used - fixed)) % max(1, amount - fixed)
        return jnp.zeros((amount,), jnp.int32).at[ranking[jnp.where(places < fixed, places, shifted)]].set(jnp.asarray(tallies, jnp.int32))

    tallies = jnp.where(number % 4 == 0, named(crowded, number // 4), named(usual, number - number // 4 - 1))
    mixed = jax.random.permutation(jax.random.fold_in(own, 3), amount)
    giver, sink = mixed[0:amount // 2 * 2:2], mixed[1:amount // 2 * 2:2]
    slack = jnp.minimum(tallies[giver] - 1, bound - tallies[sink]) // 2
    slack = jnp.where((giver == ranking[0]) | (sink == ranking[0]) | (tallies[sink] == 0), 0, jnp.maximum(slack, 0))
    shifted = jax.random.randint(jax.random.fold_in(own, 4), (amount // 2,), 0, 1 << 20) % (slack + 1)
    tallies = tallies.at[giver].add(-shifted).at[sink].add(shifted)
    members = jnp.searchsorted(jnp.cumsum(tallies), jnp.arange(rows * top), side="right").astype(jnp.int32)
    listing = members.reshape(top, rows).T
    listing = listing[jax.random.permutation(jax.random.fold_in(own, 1), rows)]
    offset_by = jax.random.randint(jax.random.fold_in(own, 2), (rows, 1), 0, top)
    return jnp.take_along_axis(listing, (jnp.arange(top)[None, :] + offset_by) % top, axis=1)


def shares(count, total, reach, lean, full):
    loads = [(1 << 20) // math.isqrt(rank ** lean) + 1 for rank in range(1, count + 1)]
    largest = reach if full else min(reach, max(-(-total // count), total * loads[0] // sum(loads)))
    least = 1 if total - largest >= count - 1 else 0
    given, rest = [largest] + [least] * (count - 1), total - largest - least * (count - 1)
    while rest > 0:
        candidates = [i for i in range(1, count) if given[i] < largest] or [i for i in range(1, count) if given[i] < reach]
        mass, remaining = sum([loads[i] for i in candidates]), rest
        for i in candidates:
            extra = min(reach - given[i], max(1, remaining * loads[i] // mass), rest)
            given[i] = given[i] + extra
            rest = rest - extra
    return np.array(given)


def bell_draw(key, dims, width, reach, pieces=(), kind=jnp.bfloat16):
    result = jax.random.normal(key, dims, jnp.float32) * width
    if len(pieces) > 0:
        result = level_of(key, dims, pieces, -0.22, 0.18) * result
    return jnp.clip(result, min=-reach, max=reach).astype(kind)


def setup_inputs(seed: int = 0) -> dict:
    keys = jax.random.split(jax.random.key(seed), 17)
    residual_in = bell_draw(keys[0], (TOKENS, D), 1.0, 6.0, ((0, 16),))
    rec_state = bell_draw(keys[1], (TOKENS, HEADS, HEAD, HEAD), 1.0, 6.0, ((0, 16), (1, 2)))
    mix_gain = jnp.clip(1.0 + 0.18 * jax.random.normal(keys[2], (D,), jnp.float32), 0.1, 1.9)
    w_query = bell_draw(keys[3], (D, D), D ** -0.5, 0.15625, ((0, 2), (1, 16)))
    w_forget = bell_draw(keys[4], (D, D), D ** -0.5, 0.15625, ((0, 2), (1, 16)))
    w_input = bell_draw(keys[5], (D, D), D ** -0.5, 0.15625, ((0, 2), (1, 16)))
    w_gate = bell_draw(keys[6], (D, D), D ** -0.5, 0.15625, ((0, 2), (1, 16)))
    lower_bound = jnp.clip(0.9 * jax.random.uniform(keys[7], (D,), jnp.float32) ** level_of(keys[7], (D,), ((0, 2),), -0.2, 0.2), 0.0, 0.9)
    head_gain = jnp.clip(1.0 + 0.18 * jax.random.normal(keys[8], (HEAD,), jnp.float32), 0.1, 1.9)
    w_out = bell_draw(keys[9], (D, D), D ** -0.5, 0.15625, ((0, 2), (1, 16)))
    ffn_gain = jnp.clip(1.0 + 0.18 * jax.random.normal(keys[10], (D,), jnp.float32), 0.1, 1.9)
    route_ids_keys = jax.random.split(jax.random.fold_in(keys[11], 1), TOKENS // SEQ_DEV)
    route_ids_turns = jax.random.permutation(jax.random.fold_in(keys[11], 3), TOKENS // SEQ_DEV)
    route_ids = jax.vmap(lambda own, number: shared_out(jax.random.fold_in(keys[11], 2), own, number, SEQ_DEV, EXPERTS, TOPK, CAP, 2))(route_ids_keys, route_ids_turns).reshape((TOKENS, TOPK))
    route_weight = jnp.clip(jnp.exp(math.log(1.0) - 1.609438 * jax.random.uniform(keys[12], (TOKENS, TOPK), jnp.float32) ** level_of(keys[12], (TOKENS, TOPK), ((0, 16),), -0.2, 0.2)), 0.2, 1.0)
    expert_gate = bell_draw(keys[13], (EXPERTS, D, FF), D ** -0.5, 0.15625, ((0, 16), (2, 2)))
    expert_up = bell_draw(keys[14], (EXPERTS, D, FF), D ** -0.5, 0.15625, ((0, 16), (2, 2)))
    expert_down = bell_draw(keys[15], (EXPERTS, FF, D), FF ** -0.5, 0.25, ((0, 16), (1, 2)))
    return dict(residual_in=residual_in, rec_state=rec_state, mix_gain=mix_gain, w_query=w_query, w_forget=w_forget, w_input=w_input, w_gate=w_gate, lower_bound=lower_bound, head_gain=head_gain, w_out=w_out, ffn_gain=ffn_gain, route_ids=route_ids, route_weight=route_weight, expert_gate=expert_gate, expert_up=expert_up, expert_down=expert_down)


rms_eps = 1e-06

def rms_scale(values, gain):
    return values * lax.rsqrt(lax.optimization_barrier(jnp.mean(values * values, axis=-1, keepdims=True)) + rms_eps) * gain

def rounded(values):
    return lax.optimization_barrier(values.astype(jnp.bfloat16)).astype(jnp.float32)

def recurrence(lower_bound, head_gain, state_block, query_raw, forget_raw, input_raw, gate_raw):
    seq_count = state_block.shape[0]
    heads_local = state_block.shape[1]
    head_size = state_block.shape[2]
    head_shape = (seq_count, heads_local, head_size)
    forget = lower_bound + (1.0 - lower_bound) * jax.nn.sigmoid(forget_raw)
    query_act = jax.nn.silu(query_raw).reshape(head_shape)
    key_act = (1.0 - forget).reshape(head_shape)
    forget_heads = forget.reshape(head_shape)
    value_act = input_raw.reshape(head_shape)
    state_next = forget_heads[:, :, :, None] * state_block.astype(jnp.float32) + key_act[:, :, :, None] * value_act[:, :, None, :]
    readout = jnp.einsum('shk,shkv->shv', query_act, state_next, precision=lax.Precision.HIGHEST)
    gate_heads = jax.nn.silu(gate_raw).reshape(head_shape)
    heads_out = rms_scale(readout, head_gain) * gate_heads
    return (state_next.astype(jnp.bfloat16), heads_out.reshape(seq_count, heads_local * head_size).astype(jnp.bfloat16))

def reference(residual_in, rec_state, mix_gain, w_query, w_forget, w_input, w_gate, lower_bound, head_gain, w_out, ffn_gain, route_ids, route_weight, expert_gate, expert_up, expert_down):
    residual = residual_in.astype(jnp.float32)
    normed = rms_scale(residual, mix_gain).astype(jnp.bfloat16)
    projected = [rounded(jnp.dot(normed, weight, preferred_element_type=jnp.float32)) for weight in (w_query, w_forget, w_input, w_gate)]

    def to_blocks(values):
        return values.reshape((N_EP, SEQ_DEV) + values.shape[1:])

    def per_block(blocks):
        return recurrence(lower_bound, head_gain, blocks[0], blocks[1], blocks[2], blocks[3], blocks[4])
    state_next, heads_out = lax.map(per_block, (to_blocks(rec_state), to_blocks(projected[0]), to_blocks(projected[1]), to_blocks(projected[2]), to_blocks(projected[3])))
    new_state = state_next.reshape(rec_state.shape)
    heads_out = heads_out.reshape(TOKENS, D)
    mixed = jnp.dot(heads_out, w_out, preferred_element_type=jnp.float32)
    after_mix = rounded(residual + mixed)
    normed_ffn = rms_scale(after_mix, ffn_gain).astype(jnp.bfloat16)

    def one_slot(slot_args):
        row_values = slot_args[0]
        expert_id = slot_args[1]
        gate_part = jnp.dot(row_values, expert_gate[expert_id], preferred_element_type=jnp.float32)
        up_part = jnp.dot(row_values, expert_up[expert_id], preferred_element_type=jnp.float32)
        hidden = (jax.nn.silu(gate_part) * up_part).astype(jnp.bfloat16)
        return jnp.dot(hidden, expert_down[expert_id], preferred_element_type=jnp.float32).astype(jnp.bfloat16)
    slot_rows = jnp.repeat(normed_ffn, TOPK, axis=0)
    expert_rows = lax.map(one_slot, (slot_rows, route_ids.reshape(-1).astype(jnp.int32)))
    expert_sum = lax.optimization_barrier(jnp.sum(route_weight[:, :, None] * expert_rows.reshape(TOKENS, TOPK, D).astype(jnp.float32), axis=1))
    layer_out = (after_mix + expert_sum).astype(jnp.bfloat16)
    return (layer_out, new_state)
```

```python
import functools

import jax
import jax.numpy as jnp
from jax import lax
from jax.experimental import pallas as pl
from jax.experimental.pallas import tpu as pltpu
from jax.sharding import PartitionSpec as P

rms_eps = 1e-06
MESH = pl.DeviceIdType.MESH
BF16 = jnp.bfloat16
F32 = jnp.float32
LANES = 128
ROWS = 16
SLOTS = 8


def rms_scale(values, gain):
    return values * lax.rsqrt(jnp.mean(values * values, axis=-1, keepdims=True) + rms_eps) * gain


def silu(values):
    return values * jax.nn.sigmoid(values)


def layer_kernel(
    n,
    tpn,
    residual_ref,
    mix_gain_ref,
    lower_ref,
    head_gain_ref,
    ffn_gain_ref,
    ids_ref,
    weight_ref,
    state_hbm,
    wq_hbm,
    wf_hbm,
    wi_hbm,
    wg_hbm,
    wo_hbm,
    eg_hbm,
    eu_hbm,
    ed_hbm,
    out_ref,
    new_hbm,
    wproj,
    wout,
    state,
    egate,
    eup,
    edown,
    resid,
    full,
    gath1,
    part2,
    recv2,
    perm,
    forget_s,
    query_s,
    value_s,
    gate_s,
    read_s,
    heads_s,
    gath3,
    part4,
    recv4,
    ids16,
    wts16,
    send5,
    recv5,
    part6,
    recv6,
    mix_s,
    load_sem,
    send_sem,
    recv_sem,
):
    me = lax.axis_index("ep")
    tp = lax.axis_index("tp")
    seq, width = residual_ref.shape
    quarter = width // tpn
    block = width // n
    nb = n // tpn
    heads = state.shape[1]

    barrier = pltpu.get_barrier_semaphore()

    def greet(i, carry):
        for j in range(tpn):
            other = lax.rem(me + i, n)
            pl.semaphore_signal(
                barrier, inc=1, device_id=(other, lax.rem(tp + j, tpn)), device_id_type=MESH
            )
        return carry

    for j in range(1, tpn):
        pl.semaphore_signal(
            barrier, inc=1, device_id=(me, lax.rem(tp + j, tpn)), device_id_type=MESH
        )
    lax.fori_loop(1, n, greet, 0)

    loads = [
        pltpu.make_async_copy(src, dst, load_sem.at[i])
        for i, (src, dst) in enumerate(
            [
                (wq_hbm, wproj.at[0]),
                (wf_hbm, wproj.at[1]),
                (wi_hbm, wproj.at[2]),
                (wg_hbm, wproj.at[3]),
                (state_hbm, state),
                (wo_hbm, wout),
                (eg_hbm, egate),
                (eu_hbm, eup),
                (ed_hbm, edown),
            ]
        )
    ]
    for load in loads:
        load.start()

    def remote(src, dst, phase, ep_to, tp_to):
        return pltpu.make_async_remote_copy(
            src_ref=src,
            dst_ref=dst,
            send_sem=send_sem.at[phase],
            recv_sem=recv_sem.at[phase],
            device_id=(ep_to, tp_to),
            device_id_type=MESH,
        )

    def drain(ref, sem):
        pltpu.make_async_copy(ref, ref, sem).wait()

    resid[...] = jnp.zeros_like(resid)
    resid[0:seq, :] = residual_ref[...].astype(F32)
    full[...] = rms_scale(resid[...], mix_gain_ref[...])
    own = pl.ds(pl.multiple_of(tp * quarter, LANES), quarter)
    gath1[me] = full[:, own].astype(BF16)

    pl.semaphore_wait(barrier, n * tpn - 1)

    def gather_start(buf, phase):
        def body(i, carry):
            remote(buf.at[me], buf.at[me], phase, lax.rem(me + i, n), tp).start()
            return carry

        lax.fori_loop(1, n, body, 0)

    gather_start(gath1, 0)

    part2[...] = jnp.zeros_like(part2)
    part4[...] = jnp.zeros_like(part4)
    read_s[...] = jnp.zeros_like(read_s)

    def perm_block(b, carry):
        lane = lax.broadcasted_iota(jnp.int32, (LANES, quarter), 0)
        col = lax.broadcasted_iota(jnp.int32, (LANES, quarter), 1)
        hit = jnp.logical_and(lane < block, col == lane + b * block)
        perm[pl.ds(pl.multiple_of(b * LANES, LANES), LANES), :] = jnp.where(hit, 1.0, 0.0).astype(
            BF16
        )
        return carry

    lax.fori_loop(0, nb, perm_block, 0)

    ids16[...] = jnp.full(ids16.shape, -1, jnp.int32)
    ids16[0:seq, :] = ids_ref[...]
    wts16[...] = jnp.zeros_like(wts16)
    wts16[0:seq, :] = weight_ref[...]
    lane8 = lax.broadcasted_iota(jnp.int32, (ROWS, n * SLOTS), 1)
    expert_of = lane8 // SLOTS
    slot_of = lane8 % SLOTS
    member = jnp.zeros((ROWS, n * SLOTS), F32)
    weighted = jnp.zeros((ROWS, n * SLOTS), F32)
    for k in range(ids_ref.shape[1]):
        same = ids16[:, k : k + 1] == expert_of
        member = member + jnp.where(same, 1.0, 0.0)
        weighted = weighted + jnp.where(same, wts16[:, k : k + 1], 0.0)
    row_i = lax.broadcasted_iota(jnp.int32, (ROWS, ROWS), 0)
    row_j = lax.broadcasted_iota(jnp.int32, (ROWS, ROWS), 1)
    earlier = jnp.where(row_j < row_i, 1.0, 0.0).astype(BF16)
    rank = jnp.dot(earlier, member.astype(BF16), preferred_element_type=F32)
    in_slot = jnp.where(rank == slot_of.astype(F32), 1.0, 0.0)
    placer = (member * in_slot).T.astype(BF16)
    weighted = weighted * in_slot
    weight_hi = weighted.astype(BF16)
    weight_lo = (weighted - weight_hi.astype(F32)).astype(BF16)

    for load in loads[:4]:
        load.wait()
    drain(gath1.at[pl.ds(0, n - 1)], recv_sem.at[0])
    rows1 = gath1[...].reshape(n * ROWS, quarter)
    for j in range(4):
        product = jnp.dot(rows1, wproj[j], preferred_element_type=F32)
        part2[:, j, :, 0:block] = product.reshape(n, ROWS, block).astype(BF16)
    target = me // nb
    place = lax.rem(me, nb)

    @pl.when(target == tp)
    def _():
        pltpu.make_async_copy(part2.at[me], recv2.at[tp, place], recv_sem.at[1]).start()

    @pl.when(target != tp)
    def _():
        remote(part2.at[me], recv2.at[tp, place], 1, me, target).start()

    def send2(i, carry):
        to = lax.rem(me + i, n)
        remote(part2.at[to], recv2.at[tp, place], 1, to, target).start()
        return carry

    lax.fori_loop(1, n, send2, 0)
    loads[4].wait()
    drain(recv2, recv_sem.at[1])
    projected = jnp.zeros((4 * ROWS, quarter), F32)
    for t in range(tpn):
        lhs = jnp.concatenate(
            [recv2[t, b].reshape(4 * ROWS, LANES) for b in range(nb)], axis=1
        )
        projected = projected + jnp.dot(lhs, perm[...], preferred_element_type=F32)
    projected = projected.astype(BF16).astype(F32)
    query_s[...] = silu(projected[0:ROWS])
    lower = lower_ref[...]
    forget_s[...] = lower + (1.0 - lower) * jax.nn.sigmoid(projected[ROWS : 2 * ROWS])
    value_s[...] = projected[2 * ROWS : 3 * ROWS]
    gate_s[...] = silu(projected[3 * ROWS : 4 * ROWS])

    def one_head(h, carry):
        cols = pl.ds(pl.multiple_of(h * LANES, LANES), LANES)
        forget_t = forget_s[:, cols].T
        query_t = query_s[:, cols].T
        for s in range(seq):
            value = value_s[s : s + 1, cols]
            updated = value + forget_t[:, s : s + 1] * (state[s, h].astype(F32) - value)
            state[s, h] = updated.astype(BF16)
            read_s[s : s + 1, cols] = jnp.sum(query_t[:, s : s + 1] * updated, 0, keepdims=True)
        heads_s[:, cols] = rms_scale(read_s[:, cols], head_gain_ref[...]) * gate_s[:, cols]
        return carry

    lax.fori_loop(0, heads, one_head, 0)
    gath3[me] = heads_s[...].astype(BF16)
    gather_start(gath3, 2)
    store = pltpu.make_async_copy(state, new_hbm, load_sem.at[9])
    store.start()

    loads[5].wait()
    drain(gath3.at[pl.ds(0, n - 1)], recv_sem.at[2])
    rows3 = gath3[...].reshape(n * ROWS, quarter)
    product = jnp.dot(rows3, wout[...], preferred_element_type=F32)
    part4[:, :, 0:block] = product.reshape(n, ROWS, block).astype(BF16)
    mine = tp * n + me
    recv4[mine] = part4[me]
    for j in range(1, tpn):
        remote(part4.at[me], recv4.at[mine], 3, me, lax.rem(tp + j, tpn)).start()

    def send4(i, carry):
        to = lax.rem(me + i, n)
        for j in range(tpn):
            remote(part4.at[to], recv4.at[mine], 3, to, lax.rem(tp + j, tpn)).start()
        return carry

    lax.fori_loop(1, n, send4, 0)
    drain(recv4.at[pl.ds(0, n * tpn - 1)], recv_sem.at[3])
    for half in range(tpn):
        mixed = jnp.zeros((ROWS, quarter), F32)
        for t in range(tpn):
            lhs = jnp.concatenate([recv4[t * n + half * nb + b] for b in range(nb)], axis=1)
            mixed = mixed + jnp.dot(lhs, perm[...], preferred_element_type=F32)
        cols = slice(half * quarter, (half + 1) * quarter)
        mix_s[:, cols] = (resid[:, cols] + mixed).astype(BF16).astype(F32)
    normed_ffn = rms_scale(mix_s[...], ffn_gain_ref[...]).astype(BF16)

    routed = jnp.dot(placer, normed_ffn, preferred_element_type=F32)
    send5[...] = routed.reshape(n, SLOTS, width).astype(BF16)
    recv5[me] = send5[me]

    def send_rows(i, carry):
        to = lax.rem(me + i, n)
        remote(send5.at[to], recv5.at[me], 4, to, tp).start()
        return carry

    lax.fori_loop(1, n, send_rows, 0)
    for load in loads[6:]:
        load.wait()
    drain(recv5.at[pl.ds(0, n - 1)], recv_sem.at[4])
    rows5 = recv5[...].astype(F32).reshape(n * SLOTS, width).astype(BF16)
    gate_part = jnp.dot(rows5, egate[0], preferred_element_type=F32)
    up_part = jnp.dot(rows5, eup[0], preferred_element_type=F32)
    hidden = (silu(gate_part) * up_part).astype(BF16)
    for t in range(tpn):
        down = jnp.dot(
            hidden, edown[0, :, t * quarter : (t + 1) * quarter], preferred_element_type=F32
        )
        part6[t] = down.reshape(n, SLOTS, quarter).astype(BF16)
    recv6[mine] = part6[tp, me]
    for j in range(1, tpn):
        to_tp = lax.rem(tp + j, tpn)
        remote(part6.at[to_tp, me], recv6.at[mine], 5, me, to_tp).start()

    def send6(i, carry):
        to = lax.rem(me + i, n)
        for j in range(tpn):
            to_tp = lax.rem(tp + j, tpn)
            remote(part6.at[to_tp, to], recv6.at[mine], 5, to, to_tp).start()
        return carry

    lax.fori_loop(1, n, send6, 0)
    drain(recv6.at[pl.ds(0, n * tpn - 1)], recv_sem.at[5])
    total = mix_s[:, own]
    for t in range(tpn):
        back = (
            recv6[t * n : (t + 1) * n].astype(F32).reshape(n * SLOTS, quarter).astype(BF16)
        )
        total = total + jnp.dot(weight_hi, back, preferred_element_type=F32)
        total = total + jnp.dot(weight_lo, back, preferred_element_type=F32)
    out_ref[...] = total[0:seq].astype(BF16)

    drain(gath1.at[pl.ds(0, n - 1)], send_sem.at[0])
    drain(part2.at[pl.ds(0, n - 1)], send_sem.at[1])

    @pl.when(target != tp)
    def _():
        drain(part2.at[0], send_sem.at[1])

    drain(gath3.at[pl.ds(0, n - 1)], send_sem.at[2])
    drain(recv4.at[pl.ds(0, n * tpn - 1)], send_sem.at[3])
    drain(send5.at[pl.ds(0, n - 1)], send_sem.at[4])
    drain(recv6.at[pl.ds(0, n * tpn - 1)], send_sem.at[5])
    store.wait()


def shards(
    residual_in,
    rec_state,
    mix_gain,
    w_query,
    w_forget,
    w_input,
    w_gate,
    lower_bound,
    head_gain,
    w_out,
    ffn_gain,
    route_ids,
    route_weight,
    expert_gate,
    expert_up,
    expert_down,
):
    tpn = lax.axis_size("tp")
    n = lax.axis_size("ep")
    seq, width = residual_in.shape
    quarter = width // tpn
    nb = n // tpn
    top = route_ids.shape[1]
    vmem = pl.BlockSpec(memory_space=pltpu.VMEM)
    hbm = pl.BlockSpec(memory_space=pl.ANY)
    rows_f32 = pltpu.VMEM((ROWS, quarter), F32)
    scratch = [
        pltpu.VMEM((4,) + w_query.shape, BF16),
        pltpu.VMEM(w_out.shape, BF16),
        pltpu.VMEM(rec_state.shape, BF16),
        pltpu.VMEM(expert_gate.shape, BF16),
        pltpu.VMEM(expert_up.shape, BF16),
        pltpu.VMEM(expert_down.shape, BF16),
        pltpu.VMEM((ROWS, width), F32),
        pltpu.VMEM((ROWS, width), F32),
        pltpu.VMEM((n, ROWS, quarter), BF16),
        pltpu.VMEM((n, 4, ROWS, LANES), BF16),
        pltpu.VMEM((tpn, nb, 4, ROWS, LANES), BF16),
        pltpu.VMEM((nb * LANES, quarter), BF16),
        rows_f32,
        rows_f32,
        rows_f32,
        rows_f32,
        rows_f32,
        rows_f32,
        pltpu.VMEM((n, ROWS, quarter), BF16),
        pltpu.VMEM((n, ROWS, LANES), BF16),
        pltpu.VMEM((tpn * n, ROWS, LANES), BF16),
        pltpu.VMEM((ROWS, top), jnp.int32),
        pltpu.VMEM((ROWS, top), F32),
        pltpu.VMEM((n, SLOTS, width), BF16),
        pltpu.VMEM((n, SLOTS, width), BF16),
        pltpu.VMEM((tpn, n, SLOTS, quarter), BF16),
        pltpu.VMEM((tpn * n, SLOTS, quarter), BF16),
        pltpu.VMEM((ROWS, width), F32),
        pltpu.SemaphoreType.DMA((10,)),
        pltpu.SemaphoreType.DMA((6,)),
        pltpu.SemaphoreType.DMA((6,)),
    ]
    return pl.pallas_call(
        functools.partial(layer_kernel, n, tpn),
        out_shape=(
            jax.ShapeDtypeStruct((seq, quarter), BF16),
            jax.ShapeDtypeStruct(rec_state.shape, BF16),
        ),
        in_specs=[vmem] * 7 + [hbm] * 9,
        out_specs=(vmem, hbm),
        scratch_shapes=scratch,
        compiler_params=pltpu.CompilerParams(
            collective_id=0, has_side_effects=True, vmem_limit_bytes=60 * 1024 * 1024
        ),
    )(
        residual_in,
        mix_gain.reshape(1, -1),
        lower_bound.reshape(1, -1),
        head_gain.reshape(1, -1),
        ffn_gain.reshape(1, -1),
        route_ids,
        route_weight,
        rec_state,
        w_query,
        w_forget,
        w_input,
        w_gate,
        w_out,
        expert_gate,
        expert_up,
        expert_down,
    )


def solution(mesh):
    in_specs = (
        P("ep", None),
        P("ep", "tp", None, None),
        P(),
        P("tp", "ep"),
        P("tp", "ep"),
        P("tp", "ep"),
        P("tp", "ep"),
        P("tp"),
        P(),
        P("tp", "ep"),
        P(),
        P("ep", None),
        P("ep", None),
        P("ep", None, "tp"),
        P("ep", None, "tp"),
        P("ep", "tp", None),
    )
    out_specs = (P("ep", "tp"), P("ep", "tp", None, None))
    return jax.shard_map(shards, mesh=mesh, in_specs=in_specs, out_specs=out_specs, check_vma=False)
```

```python
import functools

import jax
import jax.numpy as jnp
from jax import lax
from jax.experimental import pallas as pl
from jax.experimental.pallas import tpu as pltpu
from jax.sharding import PartitionSpec as P

rms_eps = 1e-06
MESH = pl.DeviceIdType.MESH
BF16 = jnp.bfloat16
F32 = jnp.float32
LANES = 128
ROWS = 16
SLOTS = 8


def rms_scale(values, gain):
    return values * lax.rsqrt(jnp.mean(values * values, axis=-1, keepdims=True) + rms_eps) * gain


def silu(values):
    return values * jax.nn.sigmoid(values)


def layer_kernel(
    n,
    tpn,
    residual_ref,
    mix_gain_ref,
    lower_ref,
    head_gain_ref,
    ffn_gain_ref,
    ids_ref,
    weight_ref,
    state_hbm,
    wq_hbm,
    wf_hbm,
    wi_hbm,
    wg_hbm,
    wo_hbm,
    eg_hbm,
    eu_hbm,
    ed_hbm,
    out_ref,
    new_ref,
    wproj,
    wraw,
    wout,
    state,
    egate,
    eup,
    edown,
    resid,
    full,
    gath1,
    part2,
    recv2,
    perm,
    forget_s,
    query_s,
    value_s,
    gate_s,
    read_s,
    heads_s,
    gath3,
    part4,
    recv4,
    ids16,
    wts16,
    send5,
    recv5,
    part6,
    recv6,
    mix_s,
    load_sem,
    send_sem,
    recv_sem,
):
    me = lax.axis_index("ep")
    tp = lax.axis_index("tp")
    seq, width = residual_ref.shape
    quarter = width // tpn
    block = width // n
    nb = n // tpn
    heads = state.shape[1]
    chips = n // 2
    wide = wproj.shape[0]
    chip = me // 2
    core = lax.rem(me, 2)
    sibling = chip * 2 + 1 - core

    barrier = pltpu.get_barrier_semaphore()

    def greet(i, carry):
        for j in range(tpn):
            other = lax.rem(me + i, n)
            pl.semaphore_signal(
                barrier, inc=1, device_id=(other, lax.rem(tp + j, tpn)), device_id_type=MESH
            )
        return carry

    for j in range(1, tpn):
        pl.semaphore_signal(
            barrier, inc=1, device_id=(me, lax.rem(tp + j, tpn)), device_id_type=MESH
        )
    lax.fori_loop(1, n, greet, 0)

    step = -(-block // 16) * 16
    if step == block:
        landing = [wproj.at[pl.ds(j * block, block)] for j in range(4)]
    else:
        landing = [wraw.at[j] for j in range(4)]
    if wide > 4 * block:
        wproj[...] = jnp.zeros_like(wproj)
    loads = [
        pltpu.make_async_copy(src, dst, load_sem.at[i])
        for i, (src, dst) in enumerate(
            [
                (wq_hbm, landing[0]),
                (wf_hbm, landing[1]),
                (wi_hbm, landing[2]),
                (wg_hbm, landing[3]),
                (state_hbm, state),
                (wo_hbm, wout),
                (eg_hbm, egate),
                (eu_hbm, eup),
                (ed_hbm, edown),
            ]
        )
    ]
    for load in loads:
        load.start()

    def remote(src, dst, phase, ep_to, tp_to):
        return pltpu.make_async_remote_copy(
            src_ref=src,
            dst_ref=dst,
            send_sem=send_sem.at[phase],
            recv_sem=recv_sem.at[phase],
            device_id=(ep_to, tp_to),
            device_id_type=MESH,
        )

    def drain(ref, sem):
        pltpu.make_async_copy(ref, ref, sem).wait()

    resid[...] = jnp.zeros_like(resid)
    resid[0:seq, :] = residual_ref[...].astype(F32)
    full[...] = rms_scale(resid[...], mix_gain_ref[...][None, :])
    own = pl.ds(pl.multiple_of(tp * quarter, LANES), quarter)
    gath1[core, chip] = full[:, own].astype(BF16)

    pl.semaphore_wait(barrier, n * tpn - 1)

    def gather_start(buf, phase):
        def body(i, carry):
            to = lax.rem(chip + i, chips) * 2 + core
            remote(buf.at[core, chip], buf.at[core, chip], phase, to, tp).start()
            return carry

        lax.fori_loop(1, chips, body, 0)

    def gather_finish(buf, phase, half_done):
        drain(buf.at[core, pl.ds(0, chips - 1)], recv_sem.at[phase])
        remote(buf.at[core], buf.at[core], phase + 1, sibling, tp).start()
        half_done(core)
        drain(buf.at[core], recv_sem.at[phase + 1])
        half_done(1 - core)

    gather_start(gath1, 0)

    part4[...] = jnp.zeros_like(part4)
    read_s[...] = jnp.zeros_like(read_s)

    def perm_block(b, carry):
        lane = lax.broadcasted_iota(jnp.int32, (LANES, quarter), 0)
        col = lax.broadcasted_iota(jnp.int32, (LANES, quarter), 1)
        hit = jnp.logical_and(lane < block, col == lane + b * block)
        perm[pl.ds(pl.multiple_of(b * LANES, LANES), LANES), :] = jnp.where(hit, 1.0, 0.0).astype(
            BF16
        )
        return carry

    lax.fori_loop(0, nb, perm_block, 0)

    ids16[...] = jnp.full(ids16.shape, -1, jnp.int32)
    ids16[:, 0:seq] = ids_ref[...]
    wts16[...] = jnp.zeros_like(wts16)
    wts16[:, 0:seq] = weight_ref[...]
    row8 = lax.broadcasted_iota(jnp.int32, (n * SLOTS, ROWS), 0)
    expert_of = row8 // SLOTS
    slot_of = row8 % SLOTS
    member = jnp.zeros((n * SLOTS, ROWS), F32)
    weighted = jnp.zeros((n * SLOTS, ROWS), F32)
    for k in range(ids_ref.shape[0]):
        same = ids16[k : k + 1, :] == expert_of
        member = member + jnp.where(same, 1.0, 0.0)
        weighted = weighted + jnp.where(same, wts16[k : k + 1, :], 0.0)
    row_i = lax.broadcasted_iota(jnp.int32, (ROWS, ROWS), 0)
    row_j = lax.broadcasted_iota(jnp.int32, (ROWS, ROWS), 1)
    earlier = jnp.where(row_i < row_j, 1.0, 0.0).astype(BF16)
    rank = jnp.dot(member.astype(BF16), earlier, preferred_element_type=F32)
    in_slot = jnp.where(rank == slot_of.astype(F32), 1.0, 0.0)
    placer = (member * in_slot).astype(BF16)
    weighted = (weighted * in_slot).T
    weight_hi = weighted.astype(BF16)
    weight_lo = (weighted - weight_hi.astype(F32)).astype(BF16)

    for load in loads[:4]:
        load.wait()
    if step != block:
        for j in range(4):
            wproj[j * step : j * step + block, :] = wraw[j]
    target = me // nb
    place = lax.rem(me, nb)

    def project(side):
        rows = gath1[side].reshape(chips * ROWS, quarter)
        product = lax.dot_general(
            rows, wproj[...], (((1,), (1,)), ((), ())), preferred_element_type=F32
        )
        part2[side] = product.reshape(chips, ROWS, wide).astype(BF16)

    gather_finish(gath1, 0, project)

    @pl.when(target == tp)
    def _():
        pltpu.make_async_copy(part2.at[core, chip], recv2.at[tp, place], recv_sem.at[6]).start()

    @pl.when(target != tp)
    def _():
        remote(part2.at[core, chip], recv2.at[tp, place], 6, me, target).start()

    def send2(i, carry):
        to = lax.rem(me + i, n)
        remote(part2.at[lax.rem(to, 2), to // 2], recv2.at[tp, place], 6, to, target).start()
        return carry

    lax.fori_loop(1, n, send2, 0)
    loads[4].wait()
    drain(recv2, recv_sem.at[6])
    blocks = recv2[...].astype(F32).reshape(n * ROWS, wide)
    shifted = []
    for j in range(4):
        moved = pltpu.roll(blocks, (wide - j * step) % wide, 1) if j else blocks
        shifted.append(moved[:, 0:LANES].astype(BF16).reshape(tpn, nb, ROWS, LANES))
    lhs = jnp.concatenate(
        [
            jnp.concatenate([shifted[j][t, b] for b in range(nb)], axis=1)
            for t in range(tpn)
            for j in range(4)
        ],
        axis=0,
    )
    placed = jnp.dot(lhs, perm[...], preferred_element_type=F32)
    placed = placed.reshape(tpn, 4 * ROWS, quarter)
    projected = placed[0]
    for t in range(1, tpn):
        projected = projected + placed[t]
    projected = projected.astype(BF16).astype(F32)
    query_s[...] = silu(projected[0:ROWS])
    lower = lower_ref[...][None, :]
    forget_s[...] = lower + (1.0 - lower) * jax.nn.sigmoid(projected[ROWS : 2 * ROWS])
    value_s[...] = projected[2 * ROWS : 3 * ROWS]
    gate_s[...] = silu(projected[3 * ROWS : 4 * ROWS])

    def one_head(h, carry):
        cols = pl.ds(pl.multiple_of(h * LANES, LANES), LANES)
        forget_t = forget_s[:, cols].T
        query_t = query_s[:, cols].T
        for s in range(seq):
            value = value_s[s : s + 1, cols]
            updated = value + forget_t[:, s : s + 1] * (state[s, h].astype(F32) - value)
            new_ref[s, h] = updated.astype(BF16)
            read_s[s : s + 1, cols] = jnp.sum(query_t[:, s : s + 1] * updated, 0, keepdims=True)
        heads_s[:, cols] = rms_scale(read_s[:, cols], head_gain_ref[...][None, :]) * gate_s[:, cols]
        return carry

    lax.fori_loop(0, heads, one_head, 0)
    gath3[core, chip] = heads_s[...].astype(BF16)
    gather_start(gath3, 2)

    loads[5].wait()

    def mix(side):
        rows = gath3[side].reshape(chips * ROWS, quarter)
        product = lax.dot_general(
            rows, wout[...], (((1,), (1,)), ((), ())), preferred_element_type=F32
        )
        part4[side, :, :, 0:block] = product.reshape(chips, ROWS, block).astype(BF16)

    gather_finish(gath3, 2, mix)
    mine = tp * n + me
    recv4[mine] = part4[core, chip]
    for j in range(1, tpn):
        remote(part4.at[core, chip], recv4.at[mine], 7, me, lax.rem(tp + j, tpn)).start()

    def send4(i, carry):
        to = lax.rem(me + i, n)
        for j in range(tpn):
            remote(
                part4.at[lax.rem(to, 2), to // 2], recv4.at[mine], 7, to, lax.rem(tp + j, tpn)
            ).start()
        return carry

    lax.fori_loop(1, n, send4, 0)
    drain(recv4.at[pl.ds(0, n * tpn - 1)], recv_sem.at[7])
    lhs = jnp.concatenate(
        [
            jnp.concatenate([recv4[t * n + half * nb + b] for b in range(nb)], axis=1)
            for t in range(tpn)
            for half in range(tpn)
        ],
        axis=0,
    )
    placed = jnp.dot(lhs, perm[...], preferred_element_type=F32)
    placed = placed.reshape(tpn, tpn, ROWS, quarter)
    for half in range(tpn):
        mixed = placed[0, half]
        for t in range(1, tpn):
            mixed = mixed + placed[t, half]
        cols = slice(half * quarter, (half + 1) * quarter)
        mix_s[:, cols] = (resid[:, cols] + mixed).astype(BF16).astype(F32)
    normed_ffn = rms_scale(mix_s[...], ffn_gain_ref[...][None, :]).astype(BF16)

    routed = jnp.dot(placer, normed_ffn, preferred_element_type=F32)
    send5[...] = routed.reshape(n, SLOTS, width).astype(BF16)
    recv5[me] = send5[me]

    def send_rows(i, carry):
        to = lax.rem(me + i, n)
        remote(send5.at[to], recv5.at[me], 4, to, tp).start()
        return carry

    lax.fori_loop(1, n, send_rows, 0)
    for load in loads[6:]:
        load.wait()
    drain(recv5.at[pl.ds(0, n - 1)], recv_sem.at[4])
    rows5 = recv5[...].astype(F32).reshape(n * SLOTS, width).astype(BF16)
    gate_part = jnp.dot(rows5, egate[0], preferred_element_type=F32)
    up_part = jnp.dot(rows5, eup[0], preferred_element_type=F32)
    hidden = (silu(gate_part) * up_part).astype(BF16)
    for t in range(tpn):
        down = jnp.dot(
            hidden, edown[0, :, t * quarter : (t + 1) * quarter], preferred_element_type=F32
        )
        part6[t] = down.reshape(n, SLOTS, quarter).astype(BF16)
    recv6[mine] = part6[tp, me]
    for j in range(1, tpn):
        to_tp = lax.rem(tp + j, tpn)
        remote(part6.at[to_tp, me], recv6.at[mine], 5, me, to_tp).start()

    def send6(i, carry):
        to = lax.rem(me + i, n)
        for j in range(tpn):
            to_tp = lax.rem(tp + j, tpn)
            remote(part6.at[to_tp, to], recv6.at[mine], 5, to, to_tp).start()
        return carry

    lax.fori_loop(1, n, send6, 0)
    drain(recv6.at[pl.ds(0, n * tpn - 1)], recv_sem.at[5])
    total = mix_s[:, own]
    for t in range(tpn):
        back = (
            recv6[t * n : (t + 1) * n].astype(F32).reshape(n * SLOTS, quarter).astype(BF16)
        )
        total = total + jnp.dot(weight_hi, back, preferred_element_type=F32)
        total = total + jnp.dot(weight_lo, back, preferred_element_type=F32)
    out_ref[...] = total[0:seq].astype(BF16)

    for buf, phase in ((gath1, 0), (gath3, 2)):
        drain(buf.at[0, pl.ds(0, chips - 1)], send_sem.at[phase])
        drain(buf.at[0], send_sem.at[phase + 1])
    drain(recv2.at[0], send_sem.at[6])
    for t in range(1, tpn - 1):
        drain(recv2.at[0], send_sem.at[6])
    drain(recv2.at[0, pl.ds(0, nb - 1)], send_sem.at[6])

    @pl.when(target != tp)
    def _():
        drain(recv2.at[0, 0], send_sem.at[6])

    drain(recv4.at[pl.ds(0, n * tpn - 1)], send_sem.at[7])
    drain(send5.at[pl.ds(0, n - 1)], send_sem.at[4])
    drain(recv6.at[pl.ds(0, n * tpn - 1)], send_sem.at[5])


def shards(
    residual_in,
    rec_state,
    mix_gain,
    w_query,
    w_forget,
    w_input,
    w_gate,
    lower_bound,
    head_gain,
    w_out,
    ffn_gain,
    route_ids,
    route_weight,
    expert_gate,
    expert_up,
    expert_down,
):
    tpn = lax.axis_size("tp")
    n = lax.axis_size("ep")
    seq, width = residual_in.shape
    quarter = width // tpn
    nb = n // tpn
    top = route_ids.shape[1]
    wide = -(-4 * (-(-width // n // 16) * 16) // LANES) * LANES
    outputs = rec_state.size * 2 + ROWS * quarter * 2
    limit = 67043328 - outputs - 8192
    vmem = pl.BlockSpec(memory_space=pltpu.VMEM)
    hbm = pl.BlockSpec(memory_space=pl.ANY)
    rows_f32 = pltpu.VMEM((ROWS, quarter), F32)
    scratch = [
        pltpu.VMEM((wide, quarter), BF16),
        pltpu.VMEM((4, width // n, quarter), BF16),
        pltpu.VMEM((width // n, quarter), BF16),
        pltpu.VMEM(rec_state.shape, BF16),
        pltpu.VMEM(expert_gate.shape, BF16),
        pltpu.VMEM(expert_up.shape, BF16),
        pltpu.VMEM(expert_down.shape, BF16),
        pltpu.VMEM((ROWS, width), F32),
        pltpu.VMEM((ROWS, width), F32),
        pltpu.VMEM((2, n // 2, ROWS, quarter), BF16),
        pltpu.VMEM((2, n // 2, ROWS, wide), BF16),
        pltpu.VMEM((tpn, nb, ROWS, wide), BF16),
        pltpu.VMEM((nb * LANES, quarter), BF16),
        rows_f32,
        rows_f32,
        rows_f32,
        rows_f32,
        rows_f32,
        rows_f32,
        pltpu.VMEM((2, n // 2, ROWS, quarter), BF16),
        pltpu.VMEM((2, n // 2, ROWS, LANES), BF16),
        pltpu.VMEM((tpn * n, ROWS, LANES), BF16),
        pltpu.VMEM((top, ROWS), jnp.int32),
        pltpu.VMEM((top, ROWS), F32),
        pltpu.VMEM((n, SLOTS, width), BF16),
        pltpu.VMEM((n, SLOTS, width), BF16),
        pltpu.VMEM((tpn, n, SLOTS, quarter), BF16),
        pltpu.VMEM((tpn * n, SLOTS, quarter), BF16),
        pltpu.VMEM((ROWS, width), F32),
        pltpu.SemaphoreType.DMA((10,)),
        pltpu.SemaphoreType.DMA((8,)),
        pltpu.SemaphoreType.DMA((8,)),
    ]
    return pl.pallas_call(
        functools.partial(layer_kernel, n, tpn),
        out_shape=(
            pltpu.VMEM((seq, quarter), BF16),
            pltpu.VMEM(rec_state.shape, BF16),
        ),
        in_specs=[vmem] * 7 + [hbm] * 9,
        out_specs=(vmem, vmem),
        scratch_shapes=scratch,
        compiler_params=pltpu.CompilerParams(
            collective_id=0, has_side_effects=True, vmem_limit_bytes=limit
        ),
    )(
        residual_in,
        mix_gain,
        lower_bound,
        head_gain,
        ffn_gain,
        route_ids.T,
        route_weight.T,
        rec_state,
        w_query.T,
        w_forget.T,
        w_input.T,
        w_gate.T,
        w_out.T,
        expert_gate,
        expert_up,
        expert_down,
    )


def solution(mesh):
    in_specs = (
        P("ep", None),
        P("ep", "tp", None, None),
        P(),
        P("tp", "ep"),
        P("tp", "ep"),
        P("tp", "ep"),
        P("tp", "ep"),
        P("tp"),
        P(),
        P("tp", "ep"),
        P(),
        P("ep", None),
        P("ep", None),
        P("ep", None, "tp"),
        P("ep", None, "tp"),
        P("ep", "tp", None),
    )
    out_specs = (P("ep", "tp"), P("ep", "tp", None, None))
    return jax.shard_map(shards, mesh=mesh, in_specs=in_specs, out_specs=out_specs, check_vma=False)
```
